512 devices in a mesh: sp: 64 (over z, y), tp: 8 (over x, core).
Axes of the slice: x: 4, y: 4, z: 16, core: 2. Of those that a mesh axis runs over, the one named last changes fastest.
Arguments:
- tokens: bfloat16 [8192, 2048], P('sp'), may hold values from -6 to 6
- in_gain: bfloat16 [2048], replicated, may hold values from 0.099609375 to 1.8984375
- w_value: bfloat16 [2048, 4096], P('sp', 'tp'), may hold values from -0.125 to 0.125
- w_gate: bfloat16 [2048, 4096], P('sp', 'tp'), may hold values from -0.125 to 0.125
- w_in_key: bfloat16 [2048, 1024], P('sp', 'tp'), may hold values from -0.125 to 0.125
- w_read: bfloat16 [2048, 1024], P('sp', 'tp'), may hold values from -0.125 to 0.125
- w_step_fwd: bfloat16 [2048, 64], P('sp', 'tp'), may hold values from -0.25 to 0.25
- w_step_bwd: bfloat16 [2048, 64], P('sp', 'tp'), may hold values from -0.25 to 0.25
- conv_value: bfloat16 [5, 4096], P(None, 'tp'), may hold values from -2.5 to 2.5
- conv_key: bfloat16 [5, 1024], P(None, 'tp'), may hold values from -2.5 to 2.5
- conv_read: bfloat16 [5, 1024], P(None, 'tp'), may hold values from -2.5 to 2.5
- step_bias: float32 [2, 64], P(None, 'tp'), may hold values from -4 to -2
- rate: float32 [2, 64], P(None, 'tp'), may hold values from 0 to 1, as said below
- norm_gain: bfloat16 [4096], P('tp'), may hold values from 0.099609375 to 1.8984375
- w_out: bfloat16 [4096, 2048], P('tp', 'sp'), may hold values from -0.09375 to 0.09375
Outputs:
- mixed: bfloat16 [8192, 2048], P('sp')
The draws below stay inside these ranges and needn't reach their ends.
Inputs may be any that keep to these rules, and one draw needn't show every extreme that they name: `rate`: positive decay rates, one per head and direction.
All inputs are finite; a program needn't handle non-finite values.
Results may differ from the reference program's by a relative error of at most 0.018.
Values may be sent and summed in bfloat16 or wider, within the bound.
A program may use at most 128 MiB of HBM per device.

```python
import math
import jax
import jax.numpy as jnp
from jax import lax

D = 2048
HEADS = 64
HEAD_DIM = 64
GROUPS = 8
STATE = 128
KERNEL = 5
BLOCK = 128
INNER = 4096
SEQ = 8192
N_TP = 8


def draw_rate(key, part):
    chooser, fast_key, slow_key = jax.random.split(jax.random.fold_in(key, 7), 3)
    fast_share = 0.5
    picked = jax.random.uniform(chooser, (2, HEADS), jnp.float32) < fast_share
    fast_rates = jnp.exp(jax.random.uniform(fast_key, (2, HEADS), jnp.float32, math.log(0.01), math.log(1.0 / 30.0))) / 0.4
    slow_rates = jnp.exp(jax.random.uniform(slow_key, (2, HEADS), jnp.float32, math.log(0.5), math.log(2.0))) / (0.4 * SEQ)
    return jnp.where(picked, fast_rates, slow_rates).astype(jnp.float32)


def steps_of(own_key, extent, pieces, smallest, largest):
    loudness = 1.0
    for position, blocks in pieces:
        steps = jax.random.uniform(jax.random.fold_in(jax.random.fold_in(own_key, 6), position), (blocks,), jnp.float32, smallest / len(pieces), largest / len(pieces))
        loudness = loudness * jnp.repeat(jnp.exp(steps), extent[position] // blocks).reshape((-1,) + (1,) * (len(extent) - 1 - position))
    return loudness


def bell_draw(own_key, dims, deviation, limit, cuts=(), dtype=jnp.bfloat16):
    entries = deviation * jax.random.normal(own_key, dims, jnp.float32)
    if cuts:
        entries = entries * steps_of(own_key, dims, cuts, -0.22, 0.18)
    return jnp.clip(entries, -limit, limit).astype(dtype)


def setup_inputs(seed: int = 0) -> dict:
    seeds = jax.random.split(jax.random.key(seed), 16)
    return {
        "tokens": bell_draw(seeds[0], (SEQ, D), 1.0, 6.0, ((0, 64),)),
        "in_gain": jnp.clip(1.0 + 0.18 * jax.random.normal(seeds[1], (D,), jnp.float32), 0.099609375, 1.8984375).astype(jnp.bfloat16),
        "w_value": bell_draw(seeds[2], (D, INNER), D ** -0.5, 0.125, ((0, 64), (1, 8))),
        "w_gate": bell_draw(seeds[3], (D, INNER), D ** -0.5, 0.125, ((0, 64), (1, 8))),
        "w_in_key": bell_draw(seeds[4], (D, GROUPS * STATE), D ** -0.5, 0.125, ((0, 64), (1, 8))),
        "w_read": bell_draw(seeds[5], (D, GROUPS * STATE), D ** -0.5, 0.125, ((0, 64), (1, 8))),
        "w_step_fwd": bell_draw(seeds[6], (D, HEADS), (D // 4) ** -0.5, 0.25, ((0, 64), (1, 8))),
        "w_step_bwd": bell_draw(seeds[7], (D, HEADS), (D // 4) ** -0.5, 0.25, ((0, 64), (1, 8))),
        "conv_value": bell_draw(seeds[8], (KERNEL, INNER), KERNEL ** -0.5, 2.5, ((1, 8),)),
        "conv_key": bell_draw(seeds[9], (KERNEL, GROUPS * STATE), KERNEL ** -0.5, 2.5, ((1, 8),)),
        "conv_read": bell_draw(seeds[10], (KERNEL, GROUPS * STATE), KERNEL ** -0.5, 2.5, ((1, 8),)),
        "step_bias": jnp.clip(-4.0 + 2.0 * jax.random.uniform(seeds[11], (2, HEADS), jnp.float32) ** steps_of(seeds[11], (2, HEADS), ((1, 8),), -0.2, 0.2), -4.0, -2.0),
        "rate": draw_rate(jax.random.fold_in(seeds[15], 71), 0),
        "norm_gain": jnp.clip(1.0 + 0.18 * jax.random.normal(seeds[13], (INNER,), jnp.float32), 0.099609375, 1.8984375).astype(jnp.bfloat16),
        "w_out": bell_draw(seeds[14], (INNER, D), INNER ** -0.5, 0.09375, ((0, 8), (1, 64))),
    }


EPSILON = 1e-05
FULL_PRECISION = lax.Precision.HIGHEST

def normalize(tensor, gain):
    return tensor * lax.rsqrt(lax.optimization_barrier(jnp.mean(tensor * tensor, -1, keepdims=True)) + EPSILON) * gain

def centred(projected, kernel_taps):
    tap_count = kernel_taps.shape[0]
    half_reach = (tap_count - 1) // 2
    length = projected.shape[0]
    padded = jnp.pad(projected.astype(jnp.float32), ((half_reach, half_reach), (0, 0)))
    summed = jnp.zeros(projected.shape, jnp.float32)
    for offset in range(tap_count):
        summed = summed + padded[offset:offset + length] * kernel_taps[offset].astype(jnp.float32)
    return jax.nn.silu(summed).astype(jnp.bfloat16)

def block_parts(values, step_size, log_decay, in_keys):
    per_group = values.shape[1] // in_keys.shape[1]
    cumulative = jnp.cumsum(log_decay, axis=0)
    log_total = cumulative[-1]
    weighting = jnp.exp(log_total[None, :] - cumulative) * step_size
    key_heads = jnp.repeat(in_keys.astype(jnp.float32), per_group, axis=1)
    scaled = (values.astype(jnp.float32) * weighting[:, :, None]).astype(jnp.bfloat16).astype(jnp.float32)
    injected = jnp.einsum('jhn,jhp->hpn', key_heads, scaled, precision=FULL_PRECISION)
    return (cumulative, jnp.exp(log_total), injected)

def block_step(memory, inputs):
    values, step_size, log_decay, in_keys, read_in = inputs
    per_group = values.shape[1] // in_keys.shape[1]
    cumulative, damping, injected = block_parts(values, step_size, log_decay, in_keys)
    scores = jnp.einsum('ign,jgn->ijg', read_in.astype(jnp.float32), in_keys.astype(jnp.float32), precision=FULL_PRECISION)
    scores = jnp.repeat(scores, per_group, axis=2)
    length = values.shape[0]
    below_mask = (jnp.arange(length)[:, None] >= jnp.arange(length)[None, :])[:, :, None]
    gaps = jnp.where(below_mask, cumulative[:, None, :] - cumulative[None, :, :], -jnp.inf)
    weights = (scores * jnp.exp(gaps) * step_size[None, :, :]).astype(jnp.bfloat16).astype(jnp.float32)
    within = jnp.einsum('ijh,jhp->ihp', weights, values.astype(jnp.float32), precision=FULL_PRECISION)
    read_heads = jnp.repeat(read_in.astype(jnp.float32), per_group, axis=1)
    carried = jnp.einsum('ihn,hpn->ihp', read_heads, memory, precision=FULL_PRECISION) * jnp.exp(cumulative)[:, :, None]
    memory = damping[:, None, None] * memory + injected
    return (memory, within + carried)

def sweep(values, step_size, log_decay, in_keys, read_in, memory):
    blocks = values.shape[0] // BLOCK

    def blocked(tensor):
        return tensor.reshape((blocks, BLOCK) + tensor.shape[1:])
    memory, swept = lax.scan(block_step, memory, (blocked(values), blocked(step_size), blocked(log_decay), blocked(in_keys), blocked(read_in)))
    return (swept.reshape((blocks * BLOCK,) + swept.shape[2:]), memory)

def reference(tokens, in_gain, w_value, w_gate, w_in_key, w_read, w_step_fwd, w_step_bwd, conv_value, conv_key, conv_read, step_bias, rate, norm_gain, w_out):
    normed = normalize(tokens.astype(jnp.float32), in_gain.astype(jnp.float32)).astype(jnp.bfloat16)

    def project(weight):
        return jnp.dot(normed, weight, preferred_element_type=jnp.float32).astype(jnp.bfloat16)
    length = tokens.shape[0]
    values = centred(project(w_value), conv_value).reshape(length, HEADS, HEAD_DIM)
    gate_raw = project(w_gate)
    in_keys = centred(project(w_in_key), conv_key).reshape(length, GROUPS, STATE)
    read_in = centred(project(w_read), conv_read).reshape(length, GROUPS, STATE)
    blank = jnp.zeros((HEADS, HEAD_DIM, STATE), jnp.float32)
    summed_heads = jnp.zeros((length, HEADS, HEAD_DIM), jnp.float32)
    for direction, weight in ((0, w_step_fwd), (1, w_step_bwd)):
        step_pre = project(weight).astype(jnp.float32)
        step_size = jax.nn.softplus(step_pre + step_bias[direction].astype(jnp.float32))
        log_decay = -rate[direction].astype(jnp.float32) * step_size
        if direction == 0:
            swept, final_state = sweep(values, step_size, log_decay, in_keys, read_in, blank)
        else:
            swept, final_state = sweep(values[::-1], step_size[::-1], log_decay[::-1], in_keys[::-1], read_in[::-1], blank)
            swept = swept[::-1]
        summed_heads = summed_heads + swept
    gated_out = summed_heads * jax.nn.silu(gate_raw.astype(jnp.float32)).reshape(length, HEADS, HEAD_DIM)
    head_gain = norm_gain.astype(jnp.float32).reshape(HEADS, HEAD_DIM)
    normed_heads = normalize(gated_out, head_gain).astype(jnp.bfloat16).reshape(length, INNER)
    part_width = INNER // N_TP
    result = jnp.zeros((length, D), jnp.float32)
    for tp_part in range(N_TP):
        portion = jnp.dot(normed_heads[:, tp_part * part_width:(tp_part + 1) * part_width], w_out[tp_part * part_width:(tp_part + 1) * part_width], preferred_element_type=jnp.float32)
        result = result + lax.optimization_barrier(portion.astype(jnp.bfloat16)).astype(jnp.float32)
    return result.astype(jnp.bfloat16)
```

```python
import functools

import jax
import jax.numpy as jnp
from jax import lax
from jax.experimental import pallas as pl
from jax.experimental.pallas import tpu as pltpu
from jax.sharding import Mesh
from jax.sharding import PartitionSpec as P

MESH = pl.DeviceIdType.MESH
F32 = jnp.float32
BF16 = jnp.bfloat16
EPS = 1e-05
L = 128
HD = 64
KERNEL = 5
SP = ("z", "y")
TP = ("x", "c")


def dot(a, b):
    return jnp.dot(a, b, preferred_element_type=F32)


def dot_nt(a, b):
    return lax.dot_general(a, b, (((1,), (1,)), ((), ())), preferred_element_type=F32)


def iota(shape, dim):
    return lax.broadcasted_iota(jnp.int32, shape, dim)


def send(src, dst, ss, rs, dev):
    return pltpu.make_async_remote_copy(
        src_ref=src, dst_ref=dst, send_sem=ss, recv_sem=rs, device_id=dev, device_id_type=MESH
    )


def silu(x):
    return x / (1.0 + jnp.exp(-x))


def softplus(x):
    return jnp.maximum(x, 0.0) + jnp.log1p(jnp.exp(-jnp.abs(x)))


def kernel(dims, *refs):
    Z, Y, X, C, D, DR = dims
    (tok, gain, wv, wg, wk, wr, wsf, wsb, wo, cv, ck, cr, bias, rate, ngain,
     out,
     slab, normed, hs, hr, w1, wfull, wot, rawp, krs, krall, kmat, rmat, ktr, vals,
     cfin, cT, sT, ecar, tots, totr, sst, srv, hf, hb, hst, hrv, yw, ast, arv,
     pbuf, prv, qbuf, xrv,
     s1_s, s1_r, tk_s, tk_r, rg_s, rg_r, hl_s, hl_r, kr_s, kr_r, tt_s, tt_r, ss_s, ss_r,
     hh_s, hh_r, aa_s, aa_r, wy_s, wy_r, dp_s, dp_r, xr_s, xr_r, xg_s, xg_r, dg_s, dg_r) = refs
    T = Y * L
    DH = D // C
    NS = L // Z
    PR = L // (X * C)
    z, y, x, c = (lax.axis_index(a) for a in ("z", "y", "x", "c"))
    up = lambda i, n, k: lax.rem(i + k, n)
    dn = lambda i, n, k: lax.rem(i + n - k, n)
    zr, zl = up(z, Z, 1), dn(z, Z, 1)
    yr, yl, yo = up(y, Y, 1), dn(y, Y, 1), up(y, Y, 2)
    oc = 1 - c
    lane = iota((1, L), 1)
    sent = []

    def go(*a):
        copy = send(*a)
        copy.start()
        sent.append(copy)

    barrier = pltpu.get_barrier_semaphore()
    near = [{"y": up(y, Y, k)} for k in range(1, Y)] + [{"x": up(x, X, k)} for k in range(1, X)]
    near += [{"z": zr}] + ([{"z": zl}] if Z > 2 else []) + ([{"c": oc}] if C > 1 else [])
    for dev in near:
        pl.semaphore_signal(barrier, inc=1, device_id=dev, device_id_type=MESH)

    onef = (iota((8, L), 1) == iota((8, L), 0) + HD).astype(BF16)
    oneb = (iota((8, L), 1) == iota((8, L), 0) + HD + 8).astype(BF16)
    if wsf.shape[1] != 8:
        n = wsf.shape[1]
        onef = (iota((n, L), 1) == iota((n, L), 0) + HD).astype(BF16)
        oneb = (iota((n, L), 1) == iota((n, L), 0) + HD + 8).astype(BF16)
    steps = dot(wsf[...], onef) + dot(wsb[...], oneb)
    kf, rf = wk[...].astype(F32), wr[...].astype(F32)
    parts = (kf, pltpu.roll(kf, HD, 1), rf, pltpu.roll(rf, HD, 1))
    for j in range(Y):
        w1[j, :, 0:L] = wv[:, j * L : (j + 1) * L]
        w1[j, :, L : 2 * L] = wg[:, j * L : (j + 1) * L]
        w1[j, :, 2 * L :] = jnp.where(lane < HD, parts[j], steps).astype(BF16)
    wfull[z, y] = w1[y]
    eye = (iota((DR, DR), 0) == iota((DR, DR), 1)).astype(BF16)
    wot[z, y] = dot_nt(eye, wo[...]).astype(BF16)
    slab[y] = tok[...]
    pl.semaphore_wait(barrier, len(near))

    for k in range(1, Y):
        go(w1.at[up(y, Y, k)], wfull.at[z, y], s1_s.at[k], s1_r.at[k], {"y": up(y, Y, k)})
    cs = pl.ds(pl.multiple_of(c * DH, DH), DH)
    go(tok.at[:, cs], slab.at[y, :, cs], tk_s.at[0], tk_r.at[0], {"y": yr})
    go(tok.at[:, cs], slab.at[y, :, cs], tk_s.at[1], tk_r.at[1], {"y": yl})

    half = Z // 2

    def blk(k, zz):
        return wot.at[zz, y] if k == 4 else wfull.at[zz, dn(y, Y, k)]

    def count(d, k):
        return half if (d == 0) == (k in (0, 1, 4)) else half - 1

    def ring(s):
        for k in range(5):
            for d in (0, 1):
                zz = dn(z, Z, s) if d == 0 else up(z, Z, s)
                ref = blk(k, zz)
                dev = {"z": zr if d == 0 else zl}
                if s == 0:
                    if d == 0 and 0 < k < 4:
                        send(ref, ref, s1_s.at[k], s1_r.at[k], {"y": yr}).wait_recv()
                elif s - 1 < count(d, k):
                    send(ref, ref, rg_s.at[d, s - 1, k], rg_r.at[d, s - 1, k], dev).wait_recv()
                if s < count(d, k):
                    go(ref, ref, rg_s.at[d, s, k], rg_r.at[d, s, k], dev)

    def tokens_one():
        lo, hi = pl.ds(0, L // 2), pl.ds(L // 2, L // 2)
        ref = slab.at[yl, :, cs]
        send(ref, ref, tk_s.at[0], tk_r.at[0], {"y": yr}).wait_recv()
        go(slab.at[yl, lo, cs], slab.at[yl, lo, cs], tk_s.at[2], tk_r.at[2], {"y": yr})
        if C > 1:
            go(ref, ref, tk_s.at[4], tk_r.at[4], {"c": oc})
        ref = slab.at[yr, :, cs]
        send(ref, ref, tk_s.at[1], tk_r.at[1], {"y": yl}).wait_recv()
        go(slab.at[yr, hi, cs], slab.at[yr, hi, cs], tk_s.at[3], tk_r.at[3], {"y": yl})
        if C > 1:
            go(ref, ref, tk_s.at[5], tk_r.at[5], {"c": oc})

    def tokens_two():
        for i, rows in ((2, pl.ds(0, L // 2)), (3, pl.ds(L // 2, L // 2))):
            ref = slab.at[yo, rows, cs]
            send(ref, ref, tk_s.at[i], tk_r.at[i], {"y": yr}).wait_recv()
        if C > 1:
            ref = slab.at[yo, :, cs]
            go(ref, ref, tk_s.at[6], tk_r.at[6], {"c": oc})

    def tokens_three():
        if C > 1:
            co = pl.ds(pl.multiple_of(oc * DH, DH), DH)
            for i, b in ((4, yl), (5, yr), (6, yo)):
                ref = slab.at[b, :, co]
                send(ref, ref, tk_s.at[i], tk_r.at[i], {"c": oc}).wait_recv()
        hs[0] = slab[Y - 1, L - 16 :, :].astype(F32)[8:].astype(BF16)
        hs[1] = slab[0, 0:16, :].astype(F32)[:8].astype(BF16)
        go(hs.at[0], hr.at[0], hl_s.at[0], hl_r.at[0], {"z": zr})
        go(hs.at[1], hr.at[1], hl_s.at[1], hl_r.at[1], {"z": zl})

    def norm(v):
        v = v.astype(F32)
        return v * lax.rsqrt(jnp.mean(v * v, -1, keepdims=True) + EPS) * gain[...].astype(F32)

    def normalize():
        def tile(i, carry):
            r = pl.multiple_of(i * 32, 32)
            normed[pl.ds(r, 32), :] = norm(slab[lax.div(i, 4), pl.ds(lax.rem(i, 4) * 32, 32), :]).astype(BF16)
            return carry
        lax.fori_loop(0, T // 32, tile, 0)

    last = max(half - 1, 0)
    for s in range(half + 1):
        ring(s)
        if s == min(3, last):
            tokens_one()
        if s == min(5, last):
            tokens_two()
        if s == min(7, last):
            tokens_three()
            normalize()

    for i in (0, 1):
        send(hr.at[i], hr.at[i], hl_s.at[i], hl_r.at[i], {"z": zr}).wait_recv()
    go(wot.at[:, y], wot.at[:, y], wy_s.at[0], wy_r.at[0], {"y": yr})
    go(wot.at[:, y], wot.at[:, y], wy_s.at[1], wy_r.at[1], {"y": yl})

    hn = jnp.concatenate([norm(hr[0]), norm(hr[1])], axis=0).astype(BF16)
    w = wfull[...].reshape(D, 3 * L)
    rh = dot(hn, w).astype(BF16).astype(F32)
    rawp[0:8, :] = jnp.where(z > 0, rh[0:8], 0.0)
    rawp[T + 8 :, :] = jnp.where(z < Z - 1, rh[8:16], 0.0)

    def project(b, carry):
        r = pl.multiple_of(b * L, L)
        rawp[pl.ds(r + 8, L), :] = dot(normed[pl.ds(r, L), :], wfull[...].reshape(D, 3 * L)).astype(BF16).astype(F32)
        return carry
    lax.fori_loop(0, Y, project, 0)

    def conv(lo, taps):
        acc = rawp[6 : 6 + T, lo : lo + L] * taps[0:1]
        for k in range(1, KERNEL):
            acc = acc + rawp[6 + k : 6 + k + T, lo : lo + L] * taps[k : k + 1]
        return silu(acc).astype(BF16)

    taps = jnp.where(y < 2, ck[...].astype(F32), cr[...].astype(F32))
    taps = jnp.where(lax.rem(y, 2) == 1, pltpu.roll(taps, HD, 1), taps)
    kr = conv(2 * L, taps).astype(F32)
    krs[...] = jnp.where(lane < HD, kr[: T // 2], pltpu.roll(kr[T // 2 :], HD, 1)).astype(BF16)
    for k in range(1, Y):
        go(krs, krall.at[y], kr_s.at[k], kr_r.at[k], {"y": up(y, Y, k)})
    krall[y] = krs[...]

    pre = pltpu.roll(rawp[8 : 8 + T, 2 * L :], lax.rem(HD + L - 2 * y, L), 1)

    def row(ref):
        val = jnp.zeros((1, L), F32)
        for d in (0, 1):
            for h in (0, 1):
                val = jnp.where(lane == 8 * d + h, ref[d, 2 * y + h], val)
        return val
    step = softplus(pre + row(bias))
    ld = -row(rate) * step
    hi = ld.astype(BF16)
    rest = ld - hi.astype(F32)
    mid = rest.astype(BF16)
    low = (rest - mid.astype(F32)).astype(BF16)
    tri = (iota((T, T), 1) <= iota((T, T), 0)).astype(BF16)
    cum = dot(tri, hi) + dot(tri, mid) + dot(tri, low)
    tot = cum[T - 1 : T]
    cfin[...] = jnp.where(lane < 8, cum, tot - cum + ld)
    cT[...] = cfin[...].T
    sT[...] = step.T
    ecar[...] = jnp.exp(cfin[...])
    damp = jnp.exp(tot)

    def spread(m, l):
        return jnp.where(lane < HD, m[:, l : l + 1], m[:, l + 1 : l + 2])
    tots[...] = jnp.concatenate([jnp.broadcast_to(spread(damp, 0), (4, L)), jnp.broadcast_to(spread(damp, 8), (4, L))], axis=0)
    for k in range(1, Z):
        go(tots, totr.at[z], tt_s.at[k], tt_r.at[k], {"z": up(z, Z, k)})
    totr[z] = tots[...]

    wdec = jnp.exp(tot - cfin[...]) * step
    vals[...] = conv(0, cv[:, pl.ds(pl.multiple_of(y * L, L), L)].astype(F32))
    vf = vals[...].astype(F32)
    scaled = [(vf * spread(wdec, l)).astype(BF16) for l in (0, 8)]

    for k in range(1, Y):
        ref = krall.at[dn(y, Y, k)]
        send(krs, ref, kr_s.at[k], kr_r.at[k], {"y": yr}).wait_recv()
    for m, i in ((kmat, 0), (rmat, 2)):
        a, b = krall[i].astype(F32), krall[i + 1].astype(F32)
        m[0 : T // 2] = jnp.where(lane < HD, a, pltpu.roll(b, HD, 1)).astype(BF16)
        m[T // 2 :] = jnp.where(lane < HD, pltpu.roll(a, HD, 1), b).astype(BF16)
    ktr[...] = kmat[...].astype(F32).T.astype(BF16)
    sf, sb = dot(ktr[...], scaled[0]), dot(ktr[...], scaled[1])
    sst[...] = jnp.concatenate([sf.reshape(Z, NS, L), sb.reshape(Z, NS, L)], axis=1).astype(BF16)
    for k in range(1, Z):
        to = up(z, Z, k)
        go(sst.at[to], srv.at[z], ss_s.at[k], ss_r.at[k], {"z": to})
    srv[z] = sst[z]

    lo, hi = pl.ds(0, half), pl.ds(half, half)
    for i, b in ((0, yl), (1, yr)):
        ref = wot.at[:, b]
        send(ref, ref, wy_s.at[i], wy_r.at[i], {"y": yr}).wait_recv()
    go(wot.at[lo, yl], wot.at[lo, yl], wy_s.at[2], wy_r.at[2], {"y": yr})
    go(wot.at[hi, yr], wot.at[hi, yr], wy_s.at[3], wy_r.at[3], {"y": yl})

    def within(b, carry):
        r = pl.multiple_of(b * L, L)
        sc = dot(rmat[pl.ds(r, L), :], ktr[...])
        i, j = iota((L, T), 0) + r, iota((L, T), 1)
        ci = cfin[pl.ds(r, L), :]
        ys = []
        for h in (0, 1):
            gap = jnp.where(j <= i, ci[:, h : h + 1] - cT[h : h + 1, :], ci[:, 8 + h : 9 + h] - cT[8 + h : 9 + h, :])
            fw, bw = sT[h : h + 1, :], sT[8 + h : 9 + h, :]
            weight = jnp.where(j < i, fw, jnp.where(j > i, bw, fw + bw))
            ys.append(dot((sc * jnp.exp(gap) * weight).astype(BF16), vals[...]))
        yw[pl.ds(r, L), :] = jnp.where(lane < HD, ys[0], ys[1])
        return carry
    lax.fori_loop(0, Y, within, 0)

    for k in range(1, Z):
        fr = dn(z, Z, k)
        send(tots, totr.at[fr], tt_s.at[k], tt_r.at[k], {"z": fr}).wait_recv()
        send(sst.at[fr], srv.at[fr], ss_s.at[k], ss_r.at[k], {"z": fr}).wait_recv()
    h = jnp.zeros((NS, L), F32)
    for k in range(Z):
        hf[k] = h
        h = totr[k, 0:1] * h + srv[k].astype(F32)[:NS]
    h = jnp.zeros((NS, L), F32)
    for k in reversed(range(Z)):
        hb[k] = h
        h = totr[k, 4:5] * h + srv[k].astype(F32)[NS:]
    hst[...] = jnp.concatenate([hf[...], hb[...]], axis=1).astype(BF16)
    for k in range(1, Z):
        to = up(z, Z, k)
        go(hst.at[to], hrv.at[z], hh_s.at[k], hh_r.at[k], {"z": to})
    hrv[z] = hst[z]
    for k in range(1, Z):
        fr = dn(z, Z, k)
        send(hst.at[fr], hrv.at[fr], hh_s.at[k], hh_r.at[k], {"z": fr}).wait_recv()
    hm = hrv[...].astype(F32)
    hfm = hm[:, :NS].reshape(L, L).astype(BF16)
    hbm = hm[:, NS:].reshape(L, L).astype(BF16)

    cols = pl.ds(pl.multiple_of(y * L, L), L)
    ng = ngain[:, cols].astype(F32)

    def finish(b, carry):
        r = pl.multiple_of(b * L, L)
        rm = rmat[pl.ds(r, L), :]
        e = ecar[pl.ds(r, L), :]
        yy = yw[pl.ds(r, L), :] + spread(e, 0) * dot(rm, hfm) + spread(e, 8) * dot(rm, hbm)
        g = yy * silu(rawp[pl.ds(r + 8, L), L : 2 * L])
        sq = g * g
        m0 = jnp.sum(jnp.where(lane < HD, sq, 0.0), -1, keepdims=True)
        m1 = jnp.sum(jnp.where(lane < HD, 0.0, sq), -1, keepdims=True)
        ms = jnp.where(lane < HD, m0, m1) * (1.0 / HD)
        ast[b] = (g * lax.rsqrt(ms + EPS) * ng).astype(BF16)
        return carry
    lax.fori_loop(0, Y, finish, 0)
    for k in range(1, Y):
        to = up(y, Y, k)
        go(ast.at[to], arv.at[y], aa_s.at[k], aa_r.at[k], {"y": to})
    arv[y] = ast[y]

    for i, rows, b in ((2, lo, yo), (3, hi, yo)):
        ref = wot.at[rows, b]
        send(ref, ref, wy_s.at[i], wy_r.at[i], {"y": yr}).wait_recv()
    for k in range(1, Y):
        fr = dn(y, Y, k)
        send(ast.at[fr], arv.at[fr], aa_s.at[k], aa_r.at[k], {"y": fr}).wait_recv()

    a = jnp.concatenate([arv[k] for k in range(Y)], axis=1)
    zg = min(Z, 4)
    wide = zg * Y * DR

    def part(t, carry):
        wt = wot[pl.ds(t * zg, zg)].reshape(wide, Y * L)
        pbuf[:, pl.ds(pl.multiple_of(t * wide, wide), wide)] = dot_nt(a, wt).astype(BF16)
        return carry
    lax.fori_loop(0, Z // zg, part, 0)

    HR = L // C
    mine = pl.ds(pl.multiple_of(c * HR, HR), HR)
    if C > 1:
        other = pl.ds(pl.multiple_of(oc * HR, HR), HR)
        go(pbuf.at[other], prv, dp_s.at[0], dp_r.at[0], {"c": oc})
        send(prv, prv, dp_s.at[0], dp_r.at[0], {"c": oc}).wait_recv()
        qbuf[...] = (pbuf[mine, :].astype(F32) + prv[...].astype(F32)).astype(BF16).reshape(X, PR, D)
    else:
        qbuf[...] = pbuf[...].reshape(X, PR, D)
    for k in range(1, X):
        to = up(x, X, k)
        go(qbuf.at[to], xrv.at[k], xr_s.at[k], xr_r.at[k], {"x": to})
    total = qbuf[x].astype(F32)
    for k in range(1, X):
        send(xrv.at[k], xrv.at[k], xr_s.at[k], xr_r.at[k], {"x": x}).wait_recv()
        total = total + xrv[k].astype(F32)

    def rows_of(xx, cc):
        return out.at[pl.ds(pl.multiple_of(cc * HR + xx * PR, PR), PR)]
    own = rows_of(x, c)
    own[...] = total.astype(BF16)
    for k in range(1, X):
        go(own, own, xg_s.at[k], xg_r.at[k], {"x": up(x, X, k)})
    if C > 1:
        go(own, own, dg_s.at[0], dg_r.at[0], {"c": oc})
    for k in range(1, X):
        ref = rows_of(dn(x, X, k), c)
        send(ref, ref, xg_s.at[k], xg_r.at[k], {"x": x}).wait_recv()
        if C > 1:
            go(ref, ref, dg_s.at[k], dg_r.at[k], {"c": oc})
    if C > 1:
        for k in range(X):
            ref = rows_of(dn(x, X, k), oc)
            send(ref, ref, dg_s.at[k], dg_r.at[k], {"c": oc}).wait_recv()
    for copy in sent:
        copy.wait_send()


def body(dims, *args):
    Z, Y, X, C, D, DR = dims
    T, NS = Y * L, L // Z
    PR = L // (X * C)
    half = max(Z // 2, 1)
    dma = pltpu.SemaphoreType.DMA
    vm = pltpu.VMEM
    in_args = list(args)
    in_args[1] = args[1].reshape(1, -1)
    in_args[13] = args[13].reshape(1, -1)
    order = in_args[:8] + [in_args[14]] + in_args[8:14]
    spaces = [pltpu.VMEM] * 12 + [pltpu.SMEM] * 2 + [pltpu.VMEM]
    scratch = [
        vm((Y, L, D), BF16),
        vm((T, D), BF16),
        vm((2, 8, D), BF16),
        vm((2, 8, D), BF16),
        vm((Y, DR, 3 * L), BF16),
        vm((Z, Y, DR, 3 * L), BF16),
        vm((Z, Y, DR, Y * L), BF16),
        vm((T + 16, 3 * L), F32),
        vm((T // 2, L), BF16),
        vm((Y, T // 2, L), BF16),
        vm((T, L), BF16),
        vm((T, L), BF16),
        vm((L, T), BF16),
        vm((T, L), BF16),
        vm((T, L), F32),
        vm((L, T), F32),
        vm((L, T), F32),
        vm((T, L), F32),
        vm((8, L), F32),
        vm((Z, 8, L), F32),
        vm((Z, 2 * NS, L), BF16),
        vm((Z, 2 * NS, L), BF16),
        vm((Z, NS, L), F32),
        vm((Z, NS, L), F32),
        vm((Z, 2 * NS, L), BF16),
        vm((Z, 2 * NS, L), BF16),
        vm((T, L), F32),
        vm((Y, L, L), BF16),
        vm((Y, L, L), BF16),
        vm((L, D), BF16),
        vm((L // C, D), BF16),
        vm((X, PR, D), BF16),
        vm((X, PR, D), BF16),
    ]
    for shape in ((Y,), (7,), (2, half, 5), (2,), (Y,), (Z,), (Z,), (Z,), (Y,), (4,), (1,), (X,), (X,), (X,)):
        scratch += [dma(shape), dma(shape)]
    return pl.pallas_call(
        functools.partial(kernel, dims),
        out_shape=jax.ShapeDtypeStruct((L, D), BF16),
        in_specs=[pl.BlockSpec(memory_space=s) for s in spaces],
        out_specs=pl.BlockSpec(memory_space=pltpu.VMEM),
        scratch_shapes=scratch,
        compiler_params=pltpu.CompilerParams(
            collective_id=0, has_side_effects=True, vmem_limit_bytes=60 * 2**20
        ),
    )(*order)


def build(mesh, Z, Y, X, C, D):
    split = Mesh(mesh.devices.reshape(Z, Y, X, C), SP + TP)
    dims = (Z, Y, X, C, D, D // (Z * Y))
    both = P(SP, TP)
    in_specs = (
        P(SP, None), P(), both, both, both, both, both, both,
        P(None, TP), P(None, TP), P(None, TP), P(None, TP), P(None, TP), P(TP), P(TP, SP),
    )
    return jax.shard_map(
        functools.partial(body, dims), mesh=split, in_specs=in_specs, out_specs=P(SP, None), check_vma=False
    )


def solution(mesh):
    return build(mesh, 16, 4, 4, 2, 2048)
```
